32 devices in a mesh: sp: 16 (over z, y, x), tp: 2 (over core).
Axes of the slice: x: 2, y: 2, z: 4, core: 2. Of those that a mesh axis runs over, the one named last changes fastest.
Arguments:
- stream: bfloat16 [2048, 2048], P(('sp', 'tp')), may hold values from -6 to 6
- wide_head_query: bfloat16 [2048, 1024], P('sp', 'tp'), may hold values from -6 to 6
- broad_attention_lookup_vectors: bfloat16 [2048, 1024], P('sp', 'tp'), may hold values from -6 to 6
- values_wide: bfloat16 [2048, 2048], P('sp', 'tp'), may hold values from -6 to 6
- query_narrow: bfloat16 [2048, 512], P('sp', 'tp'), may hold values from -6 to 6
- keys_narrow: bfloat16 [2048, 512], P('sp', 'tp'), may hold values from -6 to 6
- values_narrow: bfloat16 [2048, 1024], P('sp', 'tp'), may hold values from -6 to 6
- gate_wide: bfloat16 [2048, 2048], P('sp', 'tp'), may hold values from -6 to 6
- gate_narrow: bfloat16 [2048, 1024], P('sp', 'tp'), may hold values from -6 to 6
- log_decay: float32 [2, 8, 2048], P(None, 'tp', 'sp'), may hold values from -1.2 to 0, as said below
- gain_wide: bfloat16 [2048], P('tp'), may hold values from 0.099609375 to 1.8984375
- gain_narrow: bfloat16 [1024], P('tp'), may hold values from 0.099609375 to 1.8984375
- out_wide: bfloat16 [2048, 2048], P('tp'), may hold values from -0.109375 to 0.109375
- out_narrow: bfloat16 [1024, 2048], P('tp'), may hold values from -0.109375 to 0.109375
- gain_mix: bfloat16 [2048], replicated, may hold values from 0.099609375 to 1.8984375
- gain_pre: bfloat16 [2048], replicated, may hold values from 0.099609375 to 1.8984375
- gain_post: bfloat16 [2048], replicated, may hold values from 0.099609375 to 1.8984375
- weight_gate: bfloat16 [2048, 5120], P('sp', 'tp'), may hold values from -0.125 to 0.125
- weight_lin: bfloat16 [2048, 5120], P('sp', 'tp'), may hold values from -0.125 to 0.125
- weight_down: bfloat16 [2048, 5120], P('sp', 'tp'), may hold values from -0.078125 to 0.078125
- taps_gate: bfloat16 [3, 5120], P(None, 'tp'), may hold values from -3 to 3
- taps_lin: bfloat16 [3, 5120], P(None, 'tp'), may hold values from -3 to 3
Outputs:
- stream_out: bfloat16 [2048, 2048], P(('sp', 'tp'))
The draws below stay inside these ranges and needn't reach their ends.
Inputs may be any that keep to these rules, and one draw needn't show every extreme that they name: `log_decay`: the natural logarithm of the factor by which one head's retained state is multiplied at one position.
All inputs are finite; a program needn't handle non-finite values.
Results may differ from the reference program's by a relative error of at most 0.023.
Values may be sent and summed in bfloat16 or wider, within the bound.
No kernel may reach another device: no remote copies, remote signals or barrier semaphores. Data moves between devices by JAX's collectives and lax.ppermute only.
A program may use at most 128 MiB of HBM per device.

```python
import math
import jax
import jax.numpy as jnp
from jax import lax

D = 2048
HEADS = 8
KW = 128
VW = 256
KN = 64
VN = 128
FF = 5120
CONV = 3
BLOCK = 128
TOKENS = 2048
N_TP = 2


def draw_log_decay(key, part):
    keys = jax.random.split(jax.random.fold_in(key, 11), 6)
    fast_share = 0.5
    fast = jax.random.uniform(keys[0], (2, HEADS, 1), jnp.float32) < fast_share
    fast_rate = jnp.exp(jax.random.uniform(keys[1], (2, HEADS, 1), jnp.float32, math.log(1.0 / 60.0), math.log(1.0 / 20.0)))
    slow_rate = jnp.exp(jax.random.uniform(keys[2], (2, HEADS, 1), jnp.float32, math.log(0.15), math.log(0.6))) / TOKENS
    forgetting_speed = jnp.where(fast, fast_rate, slow_rate)
    layer_groups_list = TOKENS // BLOCK
    multiplier_coefficient = jnp.exp(jax.random.uniform(keys[3], (2, HEADS, layer_groups_list), jnp.float32, math.log(0.5), math.log(2.0)))
    multiplier_coefficient = jnp.repeat(multiplier_coefficient, BLOCK, axis=2)
    spots = jax.random.randint(keys[4], (2, HEADS, 2), 0, TOKENS)
    layer_number_total = jnp.log(1.0 - jax.random.uniform(keys[5], (2, HEADS, 2), jnp.float32, 0.2, 0.4))
    agreeing_tally = spots[..., None] == jnp.arange(TOKENS, dtype=jnp.int32)[None, None, None, :]
    segment_span = jnp.sum(jnp.where(agreeing_tally, layer_number_total[..., None], 0.0), axis=2)
    return (-forgetting_speed * multiplier_coefficient + segment_span).astype(jnp.float32)


def steps_of(rng, extent, cuts, least, high):
    level, own = 1.0, jax.random.fold_in(rng, 6)
    for axis_at, parts in cuts:
        draws = jnp.exp(jax.random.uniform(jax.random.fold_in(own, axis_at), (parts,), jnp.float32, least / len(cuts), high / len(cuts)))
        level = level * jnp.repeat(draws, extent[axis_at] // parts).reshape([-1 if axis == axis_at else 1 for axis in range(len(extent))])
    return level


def bell_draw(stream_key, dims, deviation, bound, cuts=(), kind=jnp.bfloat16):
    values = jax.random.normal(stream_key, dims, jnp.float32) * deviation
    if len(cuts) > 0:
        values = steps_of(stream_key, dims, cuts, -0.22, 0.18) * values
    return jnp.clip(values, min=-bound, max=bound).astype(kind)


def setup_inputs(seed: int = 0) -> dict:
    seeds = jax.random.split(jax.random.key(seed), 23)
    stream = bell_draw(seeds[0], (TOKENS, D), 1.0, 6.0, ((0, 32),))
    wide_head_query = bell_draw(seeds[1], (TOKENS, HEADS * KW), 1.0, 6.0, ((0, 16), (1, 2)))
    broad_attention_lookup_vectors = bell_draw(seeds[2], (TOKENS, HEADS * KW), 1.0, 6.0, ((0, 16), (1, 2)))
    values_wide = bell_draw(seeds[3], (TOKENS, HEADS * VW), 1.0, 6.0, ((0, 16), (1, 2)))
    query_narrow = bell_draw(seeds[4], (TOKENS, HEADS * KN), 1.0, 6.0, ((0, 16), (1, 2)))
    keys_narrow = bell_draw(seeds[5], (TOKENS, HEADS * KN), 1.0, 6.0, ((0, 16), (1, 2)))
    values_narrow = bell_draw(seeds[6], (TOKENS, HEADS * VN), 1.0, 6.0, ((0, 16), (1, 2)))
    gate_wide = bell_draw(seeds[7], (TOKENS, HEADS * VW), 1.0, 6.0, ((0, 16), (1, 2)))
    gate_narrow = bell_draw(seeds[8], (TOKENS, HEADS * VN), 1.0, 6.0, ((0, 16), (1, 2)))
    log_decay = draw_log_decay(jax.random.fold_in(seeds[22], 71), 0)
    gain_wide = jnp.clip(1.0 + 0.18 * jax.random.normal(seeds[10], (HEADS * VW,), jnp.float32), 0.099609375, 1.8984375).astype(jnp.bfloat16)
    gain_narrow = jnp.clip(1.0 + 0.18 * jax.random.normal(seeds[11], (HEADS * VN,), jnp.float32), 0.099609375, 1.8984375).astype(jnp.bfloat16)
    out_wide = bell_draw(seeds[12], (HEADS * VW, D), (HEADS * (VW + VN)) ** -0.5, 0.109375, ((0, 2),))
    out_narrow = bell_draw(seeds[13], (HEADS * VN, D), (HEADS * (VW + VN)) ** -0.5, 0.109375, ((0, 2),))
    gain_mix = jnp.clip(1.0 + 0.18 * jax.random.normal(seeds[14], (D,), jnp.float32), 0.099609375, 1.8984375).astype(jnp.bfloat16)
    gain_pre = jnp.clip(1.0 + 0.18 * jax.random.normal(seeds[15], (D,), jnp.float32), 0.099609375, 1.8984375).astype(jnp.bfloat16)
    gain_post = jnp.clip(1.0 + 0.18 * jax.random.normal(seeds[16], (D,), jnp.float32), 0.099609375, 1.8984375).astype(jnp.bfloat16)
    weight_gate = bell_draw(seeds[17], (D, FF), D ** -0.5, 0.125, ((0, 16), (1, 2)))
    weight_lin = bell_draw(seeds[18], (D, FF), D ** -0.5, 0.125, ((0, 16), (1, 2)))
    weight_down = bell_draw(seeds[19], (D, FF), FF ** -0.5, 0.078125, ((0, 16), (1, 2)))
    taps_gate = bell_draw(seeds[20], (CONV, FF), 0.58, 3.0, ((1, 2),))
    taps_lin = bell_draw(seeds[21], (CONV, FF), 0.58, 3.0, ((1, 2),))
    return dict(stream=stream, wide_head_query=wide_head_query, broad_attention_lookup_vectors=broad_attention_lookup_vectors, values_wide=values_wide, query_narrow=query_narrow, keys_narrow=keys_narrow, values_narrow=values_narrow, gate_wide=gate_wide, gate_narrow=gate_narrow, log_decay=log_decay, gain_wide=gain_wide, gain_narrow=gain_narrow, out_wide=out_wide, out_narrow=out_narrow, gain_mix=gain_mix, gain_pre=gain_pre, gain_post=gain_post, weight_gate=weight_gate, weight_lin=weight_lin, weight_down=weight_down, taps_gate=taps_gate, taps_lin=taps_lin)


EPS = 1e-06
THETA = 10000.0

def rotate(block, positions):
    width = block.shape[-1]
    half = width // 2
    frequency = THETA ** (-(jnp.arange(half, dtype=jnp.float32) * 2.0 / width))
    angles = positions.astype(jnp.float32)[:, None] * frequency[None, :]
    cosine = jnp.cos(angles)[:, None, :]
    sine = jnp.sin(angles)[:, None, :]
    values = block.astype(jnp.float32)
    first = values[..., :half]
    second = values[..., half:]
    return jnp.concatenate([first * cosine - second * sine, second * cosine + first * sine], axis=-1)

def block_step(state, inputs):
    query, keys, values, log_rate = inputs
    running = jnp.cumsum(log_rate, axis=1)
    length = running.shape[1]
    index = jnp.arange(length)
    lower = (index[:, None] >= index[None, :])[None]
    spread = jnp.where(lower, jnp.exp(jnp.where(lower, running[:, :, None] - running[:, None, :], 0.0)), 0.0)
    query_f = query.astype(jnp.float32)
    values_f = values.astype(jnp.float32)
    scores = jnp.einsum('ihd,jhd->hij', query_f, keys.astype(jnp.float32), precision=lax.Precision.HIGHEST) * spread
    scores = lax.optimization_barrier(scores.astype(jnp.bfloat16)).astype(jnp.float32)
    inner = jnp.einsum('hij,jhe->ihe', scores, values_f, precision=lax.Precision.HIGHEST)
    lifted = query_f * jnp.exp(running).T[:, :, None]
    cross = jnp.einsum('ihd,hde->ihe', lifted, state, precision=lax.Precision.HIGHEST)
    tail = running[:, -1:]
    scaled = keys.astype(jnp.float32) * jnp.exp(tail - running).T[:, :, None]
    scaled = lax.optimization_barrier(scaled.astype(jnp.bfloat16)).astype(jnp.float32)
    update = jnp.einsum('jhd,jhe->hde', scaled, values_f, precision=lax.Precision.HIGHEST)
    state = state * jnp.exp(tail)[:, :, None] + update
    return (state, inner + cross)

def retain(query, keys, values, log_rate, head_dim, value_dim):
    total = query.shape[0]
    heads = query.shape[1] // head_dim
    positions = jnp.arange(total, dtype=jnp.int32)
    rotated_query = rotate(query.reshape(total, heads, head_dim), positions).astype(jnp.bfloat16)
    rotated_keys = (rotate(keys.reshape(total, heads, head_dim), positions) * head_dim ** (-0.5)).astype(jnp.bfloat16)
    layer_groups_list = total // BLOCK

    def split(array):
        return array.reshape(layer_groups_list, BLOCK, heads, array.shape[-1])
    rates = jnp.transpose(log_rate.reshape(heads, layer_groups_list, BLOCK), (1, 0, 2))
    start = jnp.zeros((heads, head_dim, value_dim), jnp.float32)
    inputs = (split(rotated_query), split(rotated_keys), split(values.reshape(total, heads, value_dim)), rates)
    _, outs = lax.scan(block_step, start, inputs)
    return outs.reshape(total, heads, value_dim)

def gate_heads(retained, gain, gate):
    mean = lax.optimization_barrier(jnp.mean(retained, axis=-1, keepdims=True))
    centred = retained - mean
    variance = lax.optimization_barrier(jnp.mean(centred * centred, axis=-1, keepdims=True))
    normed = (centred * lax.rsqrt(variance + EPS)).reshape(retained.shape[0], -1)
    return (normed * gain.astype(jnp.float32) * jax.nn.silu(gate.astype(jnp.float32))).astype(jnp.bfloat16)

def scale_rows(rows, gain):
    return rows * lax.rsqrt(lax.optimization_barrier(jnp.mean(rows * rows, axis=-1, keepdims=True)) + EPS) * gain.astype(jnp.float32)

def causal_taps(upward, taps):
    width = taps.shape[0]
    total = upward.shape[0]
    padded_rows = jnp.concatenate([jnp.zeros((width - 1, upward.shape[1]), upward.dtype), upward], axis=0).astype(jnp.float32)
    smooth = jnp.zeros((total, upward.shape[1]), jnp.float32)
    for tap_index in range(width):
        smooth = smooth + taps[tap_index].astype(jnp.float32)[None, :] * padded_rows[tap_index:tap_index + total]
    return smooth

def reference(stream, wide_head_query, broad_attention_lookup_vectors, values_wide, query_narrow, keys_narrow, values_narrow, gate_wide, gate_narrow, log_decay, gain_wide, gain_narrow, out_wide, out_narrow, gain_mix, gain_pre, gain_post, weight_gate, weight_lin, weight_down, taps_gate, taps_lin):
    wide = gate_heads(retain(wide_head_query, broad_attention_lookup_vectors, values_wide, log_decay[0], KW, VW), gain_wide, gate_wide)
    narrow = gate_heads(retain(query_narrow, keys_narrow, values_narrow, log_decay[1], KN, VN), gain_narrow, gate_narrow)
    share = HEADS // N_TP
    mixed = jnp.zeros((TOKENS, D), jnp.float32)
    for group in range(N_TP):
        lo_wide, hi_wide = (group * share * VW, (group + 1) * share * VW)
        lo_narrow, hi_narrow = (group * share * VN, (group + 1) * share * VN)
        partial_sum = jnp.dot(wide[:, lo_wide:hi_wide], out_wide[lo_wide:hi_wide], preferred_element_type=jnp.float32)
        partial_sum = partial_sum + jnp.dot(narrow[:, lo_narrow:hi_narrow], out_narrow[lo_narrow:hi_narrow], preferred_element_type=jnp.float32)
        mixed = mixed + lax.optimization_barrier(partial_sum.astype(jnp.bfloat16)).astype(jnp.float32)
    resid = lax.optimization_barrier((stream.astype(jnp.float32) + scale_rows(mixed, gain_mix)).astype(jnp.bfloat16))
    normed_in = scale_rows(resid.astype(jnp.float32), gain_pre).astype(jnp.bfloat16)
    up_gate = jnp.dot(normed_in, weight_gate, preferred_element_type=jnp.float32).astype(jnp.bfloat16)
    up_lin = jnp.dot(normed_in, weight_lin, preferred_element_type=jnp.float32).astype(jnp.bfloat16)
    smooth_gate = causal_taps(up_gate, taps_gate)
    smooth_lin = causal_taps(up_lin, taps_lin)
    hidden = (jax.nn.silu(smooth_gate) * smooth_lin).astype(jnp.bfloat16)
    units = FF // N_TP
    fed = jnp.zeros((TOKENS, D), jnp.float32)
    for group in range(N_TP):
        partial_sum = lax.dot_general(hidden[:, group * units:(group + 1) * units], weight_down[:, group * units:(group + 1) * units], (((1,), (1,)), ((), ())), preferred_element_type=jnp.float32)
        fed = fed + lax.optimization_barrier(partial_sum.astype(jnp.bfloat16)).astype(jnp.float32)
    return (resid.astype(jnp.float32) + scale_rows(fed, gain_post)).astype(jnp.bfloat16)
```

```python
import functools
import math

import jax
import jax.numpy as jnp
import numpy as np
from jax import lax
from jax.experimental import pallas as pl
from jax.experimental.pallas import tpu as pltpu
from jax.sharding import Mesh
from jax.sharding import PartitionSpec as P

KW = 128
VW = 256
KN = 64
VN = 128
BLOCK = 128


EPS = 1e-06
THETA = 10000.0


def carried_in(x, axis, join, neutral):
    place = lax.axis_index(axis)
    gathered = jax.tree.map(
        lambda a, kind: lax.all_gather(a.astype(kind), axis),
        x,
        (jnp.bfloat16, jnp.bfloat16, jnp.bfloat16, jnp.bfloat16),
    )
    state = jax.tree.map(lambda a, e: jnp.zeros_like(a) + jnp.asarray(e, a.dtype), x, neutral)

    def one(lap, state):
        return join(
            state,
            jax.tree.map(
                lambda a, own: lax.dynamic_index_in_dim(a, lap, 0, False).astype(own.dtype),
                gathered,
                x,
            ),
        )

    return lax.fori_loop(0, place, one, state)


def passed_along(value, axis, steps):
    count = lax.axis_size(axis)
    first, last = (max(0, -steps), min(count, count - steps))
    return lax.ppermute(value, axis, [(source, source + steps) for source in range(first, last)])


def rotate(block, positions):
    width = block.shape[-1]
    half = width // 2
    frequency = THETA ** (-(jnp.arange(half, dtype=jnp.float32) * 2.0 / width))
    angles = positions.astype(jnp.float32)[:, None] * frequency[None, :]
    cosine = jnp.cos(angles)[:, None, :]
    sine = jnp.sin(angles)[:, None, :]
    values = block.astype(jnp.float32)
    first = values[..., :half]
    second = values[..., half:]
    return jnp.concatenate(
        [first * cosine - second * sine, second * cosine + first * sine], axis=-1
    )


def block_step(state, inputs):
    query, keys, values, log_rate = inputs
    running = jnp.cumsum(log_rate, axis=1)
    length = running.shape[1]
    index = jnp.arange(length)
    lower = (index[:, None] >= index[None, :])[None]
    spread = jnp.where(
        lower, jnp.exp(jnp.where(lower, running[:, :, None] - running[:, None, :], 0.0)), 0.0
    )
    scores = (
        jnp.einsum("ihd,jhd->hij", query, keys, preferred_element_type=jnp.float32) * spread
    ).astype(jnp.bfloat16)
    inner = jnp.einsum("hij,jhe->ihe", scores, values, preferred_element_type=jnp.float32)
    lifted = query.astype(jnp.float32) * jnp.exp(running).T[:, :, None]
    cross = jnp.einsum("ihd,hde->ihe", lifted, state, precision=lax.Precision.HIGHEST)
    tail = running[:, -1:]
    scaled = (keys.astype(jnp.float32) * jnp.exp(tail - running).T[:, :, None]).astype(jnp.bfloat16)
    update = jnp.einsum("jhd,jhe->hde", scaled, values, preferred_element_type=jnp.float32)
    state = state * jnp.exp(tail)[:, :, None] + update
    return (state, inner + cross)


def kept_nearby_memory(query, keys, values, log_rate, head_dim, value_dim, offset):
    rows = query.shape[0]
    heads = query.shape[1] // head_dim
    positions = offset + jnp.arange(rows, dtype=jnp.int32)
    rotated_query = rotate(query.reshape(rows, heads, head_dim), positions).astype(jnp.bfloat16)
    rotated_keys = (
        rotate(keys.reshape(rows, heads, head_dim), positions) * head_dim ** (-0.5)
    ).astype(jnp.bfloat16)
    layer_groups_list = rows // BLOCK

    def split(array):
        return array.reshape(layer_groups_list, BLOCK, heads, array.shape[-1])

    rates = jnp.transpose(log_rate.reshape(heads, layer_groups_list, BLOCK), (1, 0, 2))
    start = jnp.zeros((heads, head_dim, value_dim), jnp.float32)
    inputs = (
        split(rotated_query),
        split(rotated_keys),
        split(values.reshape(rows, heads, value_dim)),
        rates,
    )
    state, outs = lax.scan(block_step, start, inputs)
    return (rotated_query, outs.reshape(rows, heads, value_dim), state)


def carried(rotated_query, log_rate, state_in):
    lifted = rotated_query.astype(jnp.float32) * jnp.exp(jnp.cumsum(log_rate, axis=1)).T[:, :, None]
    return jnp.einsum("ihd,hde->ihe", lifted, state_in, precision=lax.Precision.HIGHEST)


def gate_heads(retained, gain, gate):
    mean = jnp.mean(retained, axis=-1, keepdims=True)
    centred = retained - mean
    variance = jnp.mean(centred * centred, axis=-1, keepdims=True)
    normed = (centred * lax.rsqrt(variance + EPS)).reshape(retained.shape[0], -1)
    return (normed * gain.astype(jnp.float32) * jax.nn.silu(gate.astype(jnp.float32))).astype(
        jnp.bfloat16
    )


def scale_rows(rows, gain):
    return (
        rows
        * lax.rsqrt(jnp.mean(rows * rows, axis=-1, keepdims=True) + EPS)
        * gain.astype(jnp.float32)
    )


def causal_taps(upward, before, taps):
    width = taps.shape[0]
    total = upward.shape[0]
    padded_rows = jnp.concatenate([before, upward], axis=0).astype(jnp.float32)
    smooth = jnp.zeros((total, upward.shape[1]), jnp.float32)
    for tap_index in range(width):
        smooth = (
            smooth
            + taps[tap_index].astype(jnp.float32)[None, :]
            * padded_rows[tap_index : tap_index + total]
        )
    return smooth


def chain(earlier, later):
    return (
        earlier[0] * later[2] + later[0],
        earlier[1] * later[3] + later[1],
        earlier[2] * later[2],
        earlier[3] * later[3],
    )


def general_body(
    stream,
    wide_head_query,
    broad_attention_lookup_vectors,
    values_wide,
    query_narrow,
    keys_narrow,
    values_narrow,
    gate_wide,
    gate_narrow,
    log_decay,
    gain_wide,
    gain_narrow,
    out_wide,
    out_narrow,
    gain_mix,
    gain_pre,
    gain_post,
    weight_gate,
    weight_lin,
    weight_down,
    taps_gate,
    taps_lin,
):
    rows = wide_head_query.shape[0]
    offset = lax.axis_index("sp") * rows
    rates_wide = log_decay[0]
    rates_narrow = log_decay[1]
    rot_wide, local_wide, state_wide = kept_nearby_memory(
        wide_head_query, broad_attention_lookup_vectors, values_wide, rates_wide, KW, VW, offset
    )
    rot_narrow, local_narrow, state_narrow = kept_nearby_memory(
        query_narrow, keys_narrow, values_narrow, rates_narrow, KN, VN, offset
    )
    decay_wide = jnp.exp(jnp.sum(rates_wide, axis=1))[:, None, None]
    decay_narrow = jnp.exp(jnp.sum(rates_narrow, axis=1))[:, None, None]
    identity = (
        jnp.zeros_like(state_wide),
        jnp.zeros_like(state_narrow),
        jnp.ones_like(decay_wide),
        jnp.ones_like(decay_narrow),
    )
    incoming = carried_in(
        (state_wide, state_narrow, decay_wide, decay_narrow), "sp", chain, identity
    )
    gated_wide = gate_heads(
        local_wide + carried(rot_wide, rates_wide, incoming[0]), gain_wide, gate_wide
    )
    gated_narrow = gate_heads(
        local_narrow + carried(rot_narrow, rates_narrow, incoming[1]), gain_narrow, gate_narrow
    )
    part_wide = jnp.dot(gated_wide, out_wide, preferred_element_type=jnp.float32)
    part_narrow = jnp.dot(gated_narrow, out_narrow, preferred_element_type=jnp.float32)
    mixed = lax.psum_scatter(
        (part_wide + part_narrow).astype(jnp.bfloat16), "tp", scatter_dimension=0, tiled=True
    ).astype(jnp.float32)
    resid = (stream.astype(jnp.float32) + scale_rows(mixed, gain_mix)).astype(jnp.bfloat16)
    normed_in = scale_rows(resid.astype(jnp.float32), gain_pre).astype(jnp.bfloat16)
    normed_all = lax.all_gather(normed_in, "tp", axis=0, tiled=True)
    whole_gate, whole_lin = (
        lax.all_gather(weight_gate, "sp", axis=0, tiled=True),
        lax.all_gather(weight_lin, "sp", axis=0, tiled=True),
    )
    up_gate = jnp.dot(normed_all, whole_gate, preferred_element_type=jnp.float32).astype(
        jnp.bfloat16
    )
    up_lin = jnp.dot(normed_all, whole_lin, preferred_element_type=jnp.float32).astype(jnp.bfloat16)
    reach = taps_gate.shape[0] - 1
    before_gate, before_lin = passed_along(
        (up_gate[rows - reach :], up_lin[rows - reach :]), "sp", 1
    )
    smooth_gate = causal_taps(up_gate, before_gate, taps_gate)
    smooth_lin = causal_taps(up_lin, before_lin, taps_lin)
    hidden = (jax.nn.silu(smooth_gate) * smooth_lin).astype(jnp.bfloat16)
    terms = lax.dot_general(
        hidden,
        lax.all_gather(weight_down, "sp", axis=0, tiled=True),
        (((1,), (1,)), ((), ())),
        preferred_element_type=jnp.float32,
    )
    fed = lax.psum_scatter(
        terms.astype(jnp.bfloat16), "tp", scatter_dimension=0, tiled=True
    ).astype(jnp.float32)
    return (resid.astype(jnp.float32) + scale_rows(fed, gain_post)).astype(jnp.bfloat16)


F32 = jnp.float32
BF16 = jnp.bfloat16
LO = 4
VMEM_SPEC = pl.BlockSpec(memory_space=pltpu.VMEM)
SMEM_SPEC = pl.BlockSpec(memory_space=pltpu.SMEM)


def dot(a, b, contract=((1,), (0,)), precision=None):
    return lax.dot_general(a, b, (contract, ((), ())), precision=precision, preferred_element_type=F32)


def call(kernel, name, outs, ins, scratch=(), flops=2_000_000, vmem=48):
    return pl.pallas_call(
        kernel,
        name=name,
        out_shape=outs,
        in_specs=[SMEM_SPEC if a.dtype == jnp.int32 else VMEM_SPEC for a in ins],
        out_specs=jax.tree.map(lambda _: VMEM_SPEC, outs),
        scratch_shapes=list(scratch),
        compiler_params=pltpu.CompilerParams(vmem_limit_bytes=vmem * 2**20),
        cost_estimate=pl.CostEstimate(
            flops=flops, bytes_accessed=sum(a.size * a.dtype.itemsize for a in ins), transcendentals=0
        ),
    )(*ins)


def struct(shape, dtype=BF16):
    return jax.ShapeDtypeStruct(shape, dtype)


def iota(shape, axis):
    return lax.broadcasted_iota(jnp.int32, shape, axis)


def frequency_rows():
    lane = np.arange(128)

    def row(width):
        half = width // 2
        index = (lane % half).astype(np.float32)
        frequency = np.float32(THETA) ** (-(index * np.float32(2.0) / np.float32(width)))
        sign = np.where(lane % width < half, -1.0, 1.0)
        return [frequency.astype(np.float32), sign.astype(np.float32)]

    rows = row(KW) + row(KN)
    return np.stack(rows + [np.zeros(128, np.float32)] * 4).astype(np.float32)


def rotation(tables, start, count):
    position = (iota((count, 128), 0) + start).astype(F32)
    out = []
    for group in range(2):
        angle = position * tables[2 * group : 2 * group + 1, :]
        out.append((jnp.cos(angle), jnp.sin(angle) * tables[2 * group + 1 : 2 * group + 2, :]))
    return out


def turn_wide(values, table):
    return values * table[0] + pltpu.roll(values, KW // 2, 1) * table[1]


def turn_narrow(values, table):
    half = KN // 2
    lane = iota(values.shape, 1) % KN
    other = jnp.where(lane < half, pltpu.roll(values, 128 - half, 1), pltpu.roll(values, half, 1))
    return values * table[0] + other * table[1]


def states_kernel(place, tables, kw, kn, vw, vn, rate, cos_out, own, m1, m2, m3, pieces):
    rows = kw.shape[0]
    heads = kw.shape[1] // KW
    span = pieces.shape[1]
    unit = (span - 4 * heads) // heads
    both = rate[...].reshape(2 * heads, rows)
    later = (iota((rows, rows), 1) > iota((rows, rows), 0)).astype(F32)
    suffix = dot(later, both, ((1,), (1,)), lax.Precision.HIGHEST)
    rise = jnp.exp(suffix)
    total = dot(both, jnp.ones((rows, 128), F32), ((1,), (0,)), lax.Precision.HIGHEST)
    coarse = total.astype(BF16).astype(F32)
    marks = jnp.concatenate([coarse, total - coarse], axis=0).astype(BF16)
    wide, narrow = rotation(tables[...], place[0] * rows, rows)
    for at, value in enumerate(wide + narrow):
        cos_out[at] = value
    part_w, part_n = KW // LO, KN // LO
    for head in range(heads):
        keys = turn_wide(kw[:, head * KW : (head + 1) * KW].astype(F32), wide) * KW**-0.5
        keys = keys.astype(BF16).astype(F32)
        scaled = (keys * rise[:, head : head + 1]).astype(BF16)
        update = dot(scaled, vw[:, head * VW : (head + 1) * VW], ((0,), (0,))).astype(BF16)
        for quarter in range(LO):
            at = head * unit
            some = update[quarter * part_w : (quarter + 1) * part_w]
            for side in range(VW // 128):
                pieces[quarter, at : at + part_w, :] = some[:, side * 128 : (side + 1) * 128]
                at += part_w
    for pair in range(heads * KN // 128):
        keys = turn_narrow(kn[:, pair * 128 : (pair + 1) * 128].astype(F32), narrow) * KN**-0.5
        keys = keys.astype(BF16).astype(F32)
        first = heads + 2 * pair
        lane = iota(keys.shape, 1) < KN
        scaled = (keys * jnp.where(lane, rise[:, first : first + 1], rise[:, first + 1 : first + 2])).astype(BF16)
        update = dot(scaled, vn[:, 2 * pair * VN : 2 * (pair + 1) * VN], ((0,), (0,))).astype(BF16)
        for member in range(2):
            head = 2 * pair + member
            some = update[member * KN : (member + 1) * KN, member * VN : (member + 1) * VN]
            at = head * unit + (VW // 128) * part_w
            for quarter in range(LO):
                pieces[quarter, at : at + part_n, :] = some[quarter * part_n : (quarter + 1) * part_n]
    for quarter in range(LO):
        pieces[quarter, span - 4 * heads :, :] = marks
    for step, out in enumerate((own, m1, m2, m3)):
        out[...] = pieces[place[2] ^ step]


def near_kernel(place, tables, qw, qn, kw, kn, vw, vn, rate, inner_w, inner_n, lift_w, lift_n):
    rows = kw.shape[0]
    heads = kw.shape[1] // KW
    both = rate[...].reshape(2 * heads, rows)
    lower = iota((rows, rows), 0) >= iota((rows, rows), 1)
    upto = lower.astype(F32)
    down = dot(upto, both, ((1,), (1,)), lax.Precision.HIGHEST)
    along = dot(both, upto, ((1,), (1,)), lax.Precision.HIGHEST)
    grown = jnp.exp(down)
    wide, narrow = (tables[0], tables[1]), (tables[2], tables[3])

    def spread(at):
        gap = jnp.where(lower, down[:, at : at + 1] - along[at : at + 1, :], 0.0)
        return jnp.where(lower, jnp.exp(gap), 0.0)

    for head in range(heads):
        query = turn_wide(qw[:, head * KW : (head + 1) * KW].astype(F32), wide).astype(BF16)
        keys = (turn_wide(kw[:, head * KW : (head + 1) * KW].astype(F32), wide) * KW**-0.5).astype(BF16)
        scores = (dot(query, keys, ((1,), (1,))) * spread(head)).astype(BF16)
        inner_w[:, head * VW : (head + 1) * VW] = dot(scores, vw[:, head * VW : (head + 1) * VW])
        lift_w[:, head * KW : (head + 1) * KW] = (query.astype(F32) * grown[:, head : head + 1]).astype(BF16)
    for pair in range(heads * KN // 128):
        span = slice(pair * 128, (pair + 1) * 128)
        query = turn_narrow(qn[:, span].astype(F32), narrow).astype(BF16)
        keys = (turn_narrow(kn[:, span].astype(F32), narrow) * KN**-0.5).astype(BF16)
        lane = iota(query.shape, 1) < KN
        first = heads + 2 * pair
        for member in range(2):
            head = 2 * pair + member
            mine = jnp.where(lane if member == 0 else ~lane, query, jnp.zeros_like(query))
            scores = (dot(mine, keys, ((1,), (1,))) * spread(first + member)).astype(BF16)
            inner_n[:, head * VN : (head + 1) * VN] = dot(scores, vn[:, head * VN : (head + 1) * VN])
        both_grown = jnp.where(lane, grown[:, first : first + 1], grown[:, first + 1 : first + 2])
        lift_n[:, span] = (query.astype(F32) * both_grown).astype(BF16)


def plane_kernel(place, own, m1, m2, m3, before, decay, total, *, heads):
    body = own.shape[0] - 4 * heads
    unit = body // heads
    wide_rows = (VW // 128) * (KW // LO)
    parts = (own, m1, m2, m3)
    spot = [place[2] ^ step for step in range(LO)]
    logs = []
    for part in parts:
        marks = part[body:, :].astype(F32)
        logs.append(marks[: 2 * heads] + marks[2 * heads :])
    zero = jnp.zeros_like(logs[0])
    values = [part[:body, :].astype(F32) for part in parts]

    def between(start, end):
        out = zero
        for at, log in zip(spot, logs):
            inside = jnp.logical_and(at > start, at < end)
            out = out + jnp.where(inside, log, 0.0)
        return out

    for end in range(LO + 1):
        factors = [
            jnp.where(at < end, jnp.exp(between(at, end)), 0.0) for at in spot
        ]
        if end < LO:
            decay[end] = jnp.exp(between(-1, end))
        else:
            whole = between(-1, end)
            coarse = whole.astype(BF16).astype(F32)
            total[body:, :] = jnp.concatenate([coarse, whole - coarse], axis=0).astype(BF16)
        for head in range(heads):
            for at, stop, row in (
                (head * unit, head * unit + wide_rows, head),
                (head * unit + wide_rows, (head + 1) * unit, heads + head),
            ):
                value = sum(v[at:stop] * f[row : row + 1, :] for v, f in zip(values, factors))
                if end < LO:
                    before[end, at:stop, :] = value
                else:
                    total[at:stop, :] = value.astype(BF16)


def line_kernel(place, before, decay, *refs, heads):
    count = len(refs) - LO
    parts, outs = refs[:count], refs[count:]
    body = before.shape[1]
    unit = body // heads
    wide_rows = (VW // 128) * (KW // LO)
    mine = place[1]
    spot = [mine ^ (step + 1) for step in range(count)]
    logs = []
    for part in parts:
        marks = part[body:, :].astype(F32)
        logs.append(marks[: 2 * heads] + marks[2 * heads :])
    factors = []
    for start in spot:
        gap = jnp.zeros_like(logs[0])
        for at, log in zip(spot, logs):
            gap = gap + jnp.where(jnp.logical_and(at > start, at < mine), log, 0.0)
        factors.append(jnp.where(start < mine, jnp.exp(gap), 0.0))
    for head in range(heads):
        for at, stop, row in (
            (head * unit, head * unit + wide_rows, head),
            (head * unit + wide_rows, (head + 1) * unit, heads + head),
        ):
            value = sum(p[at:stop, :].astype(F32) * f[row : row + 1, :] for p, f in zip(parts, factors))
            for step, out in enumerate(outs):
                end = place[2] ^ step
                out[at:stop, :] = (
                    before[end, at:stop, :] + decay[end][row : row + 1, :] * value
                ).astype(BF16)


def gated(retained, gain, gate):
    mean = jnp.mean(retained, axis=-1, keepdims=True)
    centred = retained - mean
    variance = jnp.mean(centred * centred, axis=-1, keepdims=True)
    gate = gate.astype(F32)
    normed = centred * lax.rsqrt(variance + EPS) * gain.astype(F32)
    return (normed * (gate / (1.0 + jnp.exp(-gate)))).astype(BF16)


def gate_kernel(
    place, s0, s1, s2, s3, inner_w, inner_n, lift_w, lift_n, gain_w, gain_n, gate_w, gate_n, out_w, out_n, wide, narrow
):
    heads = lift_w.shape[1] // KW
    unit = s0.shape[0] // heads
    part_w, part_n = KW // LO, KN // LO
    for step, part in enumerate((s0, s1, s2, s3)):
        quarter = place[2] ^ step
        for head in range(heads):
            at = head * unit
            for side in range(VW // 128):
                wide[head, pl.ds(pl.multiple_of(quarter * part_w, part_w), part_w), side * 128 : (side + 1) * 128] = part[
                    at : at + part_w, :
                ]
                at += part_w
            where = (head % 2) * KN + quarter * part_n
            narrow[head // 2, pl.ds(pl.multiple_of(where, part_n), part_n), :] = part[at : at + part_n, :]
    for head in range(heads):
        span = slice(head * VW, (head + 1) * VW)
        retained = inner_w[:, span] + dot(lift_w[:, head * KW : (head + 1) * KW], wide[head])
        out_w[:, span] = gated(retained, gain_w[0:1, span], gate_w[:, span])
    for head in range(heads):
        pair = head // 2
        span = slice(head * VN, (head + 1) * VN)
        lifted = lift_n[:, pair * 128 : (pair + 1) * 128]
        lane = iota(lifted.shape, 1) < KN
        mine = jnp.where(lane if head % 2 == 0 else ~lane, lifted, jnp.zeros_like(lifted))
        retained = inner_n[:, span] + dot(mine, narrow[pair])
        out_n[:, span] = gated(retained, gain_n[0:1, span], gate_n[:, span])


def project_kernel(place, wide, narrow, out_wide, out_narrow, mine, theirs):
    half = wide.shape[0] // 2
    whole = dot(wide[...], out_wide[...]) + dot(narrow[...], out_narrow[...])
    first = place[3] == 0
    mine[...] = jnp.where(first, whole[:half], whole[half:])
    theirs[...] = jnp.where(first, whole[half:], whole[:half]).astype(BF16)


def norm_rows(rows):
    return rows * lax.rsqrt(jnp.mean(rows * rows, axis=-1, keepdims=True) + EPS)


def enter_kernel(mine, theirs, stream, gain_mix, gain_pre, resid, normed):
    mixed = mine[...].astype(BF16).astype(F32) + theirs[...].astype(F32)
    value = (stream[...].astype(F32) + norm_rows(mixed) * gain_mix[0:1, :].astype(F32)).astype(BF16)
    resid[...] = value
    normed[...] = (norm_rows(value.astype(F32)) * gain_pre[0:1, :].astype(F32)).astype(BF16)


def up_kernel(place, near, far, *refs, rest):
    weights, out, rows = refs[:-2], refs[-2], refs[-1]
    line = near.shape[0]
    half = near.shape[1]
    width = out.shape[-1]
    mine, other = place[3], 1 - place[3]
    acc = None
    for step in range(LO):
        spot = place[2] ^ step
        lead = []
        for turn in range(line):
            column = pl.multiple_of(((place[1] ^ turn) * LO + spot) * 128, 128)
            for source, core in ((near, mine), (far, other)):
                rows[turn, :, pl.ds(pl.multiple_of(core * half, half), half), :] = source[:, :, pl.ds(column, 128)]
        parts = [rows[turn].reshape(2 * half * line, 128) for turn in range(line)]
        first = weights[step]
        if step < LO - 1:
            later = weights[LO + step][...].reshape((line - 1) * 128, width)
            term = dot(jnp.concatenate(parts[1:], axis=1), later)
        else:
            upper, lower = weights[LO + step], weights[LO + step + 1]
            tall = upper.shape[1]
            later = jnp.concatenate([upper[...], lower[...]], axis=1).reshape((line - 1) * 128, width)
            term = dot(jnp.concatenate(parts[1:], axis=1), later)
        term = term + dot(parts[0], first[:, :width])
        acc = term if acc is None else acc + term
    out[...] = acc.astype(BF16).reshape(out.shape)


def down_kernel(place, up, halo, taps_gate, taps_lin, *refs):
    weights, (mine, theirs, hidden) = refs[:-3], refs[-3:]
    line, rows, double = up.shape
    width = double // 2
    half = rows // 2
    start = place[4] * width
    taps = []
    row = iota((rows, width), 0)
    for turn in range(line):
        where = place[1] ^ turn
        before = jnp.where(place[2] == 0, where - 1, where)
        source = place[1] ^ jnp.maximum(before, 0)
        keep = before >= 0
        sides = []
        for side, table in enumerate((taps_gate, taps_lin)):
            value = up[turn, :, side * width : (side + 1) * width].astype(F32)
            old = jnp.where(keep, halo[source, :, side * width : (side + 1) * width].astype(F32), 0.0)
            total = table[2:3, :].astype(F32) * value
            one = jnp.where(row == 0, old[1:2, :], pltpu.roll(value, 1, 0))
            two = jnp.where(row == 0, old[0:1, :], jnp.where(row == 1, old[1:2, :], pltpu.roll(value, 2, 0)))
            sides.append(table[0:1, :].astype(F32) * two + table[1:2, :].astype(F32) * one + total)
        gate, linear = sides
        value = (gate / (1.0 + jnp.exp(-gate)) * linear).astype(BF16)
        hidden[0, turn * half : (turn + 1) * half, :] = value[:half]
        hidden[1, turn * half : (turn + 1) * half, :] = value[half:]
    for target, core in ((theirs, 1 - place[3]), (mine, place[3])):
        value = hidden[core]
        for step in range(LO):
            spot = place[2] ^ step
            if step < LO - 1:
                later = weights[LO + step][...].reshape((line - 1) * 128, width)
            else:
                later = jnp.concatenate([weights[LO + step][...], weights[LO + step + 1][...]], axis=1)
                later = later.reshape((line - 1) * 128, width)
            first = weights[step][:, 2 * width :]
            pieces = [dot(value, first, ((1,), (1,)))]
            rest = dot(value, later, ((1,), (1,)))
            pieces += [rest[:, at * 128 : (at + 1) * 128] for at in range(line - 1)]
            for turn, piece in enumerate(pieces):
                column = pl.multiple_of(((place[1] ^ turn) * LO + spot) * 128, 128)
                target[:, :, pl.ds(column, 128)] = piece.reshape(line, half, 128).astype(target.dtype)


def sum_kernel(mine, theirs, *outs):
    for turn, out in enumerate(outs):
        value = mine[turn].astype(F32) + theirs[turn].astype(F32)
        out[...] = value.astype(out.dtype)


def leave_kernel(resid, gain, *refs):
    out = refs[-1]
    fed = sum(ref[...].astype(F32) for ref in refs[:-1])
    out[...] = (resid[...].astype(F32) + norm_rows(fed) * gain[0:1, :].astype(F32)).astype(BF16)


def crossed(value, axis, step):
    count = lax.axis_size(axis)
    return lax.ppermute(value, axis, [(at, at ^ step) for at in range(count)])


def shared(value, halves_axis):
    one = crossed(value, "lo", 1)
    two = crossed(value, "lo", 2)
    size = value.shape[halves_axis] // 2
    upper = crossed(lax.slice_in_dim(one, 0, size, axis=halves_axis), "lo", 2)
    lower = crossed(lax.slice_in_dim(two, size, 2 * size, axis=halves_axis), "lo", 1)
    return [one, two, upper, lower]


def fast_body(
    stream,
    wide_head_query,
    broad_attention_lookup_vectors,
    values_wide,
    query_narrow,
    keys_narrow,
    values_narrow,
    gate_wide,
    gate_narrow,
    log_decay,
    gain_wide,
    gain_narrow,
    out_wide,
    out_narrow,
    gain_mix,
    gain_pre,
    gain_post,
    weight_gate,
    weight_lin,
    weight_down,
    taps_gate,
    taps_lin,
):
    line = lax.axis_size("hi")
    rows = wide_head_query.shape[0]
    half = rows // 2
    heads = wide_head_query.shape[1] // KW
    model = stream.shape[1]
    width = weight_gate.shape[1] // line
    mine, spot, core = lax.axis_index("hi"), lax.axis_index("lo"), lax.axis_index("core")
    place = jnp.stack([mine * LO + spot, mine, spot, core, mine]).astype(jnp.int32)

    def columns(array, step):
        return lax.dynamic_slice_in_dim(array, (mine ^ step) * width, width, 1)

    body_rows = heads * ((VW // 128) * (KW // LO) + KN // LO)
    span = body_rows + 4 * heads
    packed = struct((span, 128))
    tables, *pieces = call(
        states_kernel,
        "states",
        (struct((4, rows, 128), F32),) + (packed,) * LO,
        (place, jnp.asarray(frequency_rows()), broad_attention_lookup_vectors, keys_narrow, values_wide, values_narrow, log_decay),
        [pltpu.VMEM((LO, span, 128), BF16)],
        flops=200_000_000,
    )
    moved = [crossed(pieces[step], "lo", step) for step in range(1, LO)]

    early = jnp.concatenate([columns(w, 0) for w in (weight_gate, weight_lin, weight_down)], axis=1)
    early_all = [early] + [crossed(early, "lo", step) for step in range(1, LO)]
    ups = jnp.stack(
        [
            crossed(jnp.concatenate([columns(weight_gate, step), columns(weight_lin, step)], axis=1), "hi", step)
            for step in range(1, line)
        ]
    )
    downs = jnp.stack([crossed(columns(weight_down, step), "hi", step) for step in range(1, line)])
    ups_all = [ups] + shared(ups, 1)
    downs_all = [downs] + shared(downs, 1)

    inner_w, inner_n, lift_w, lift_n = call(
        near_kernel,
        "near",
        (
            struct((rows, heads * VW), F32),
            struct((rows, heads * VN), F32),
            struct((rows, heads * KW)),
            struct((rows, heads * KN)),
        ),
        (
            place,
            tables,
            wide_head_query,
            query_narrow,
            broad_attention_lookup_vectors,
            keys_narrow,
            values_wide,
            values_narrow,
            log_decay,
        ),
        flops=400_000_000,
    )
    before, decay, total = call(
        functools.partial(plane_kernel, heads=heads),
        "plane",
        (struct((LO, body_rows, 128), F32), struct((LO, 2 * heads, 128), F32), packed),
        (place, pieces[0], *moved),
    )
    lines = [crossed(total, "hi", step) for step in range(1, line)]
    states = call(
        functools.partial(line_kernel, heads=heads),
        "line",
        (struct((body_rows, 128)),) * LO,
        (place, before, decay, *lines),
    )
    states = [states[0]] + [crossed(states[step], "lo", step) for step in range(1, LO)]
    gated_wide, gated_narrow = call(
        gate_kernel,
        "gate",
        (struct((rows, heads * VW)), struct((rows, heads * VN))),
        (
            place,
            *states,
            inner_w,
            inner_n,
            lift_w,
            lift_n,
            gain_wide[None],
            gain_narrow[None],
            gate_wide,
            gate_narrow,
        ),
        [pltpu.VMEM((heads, KW, VW), BF16), pltpu.VMEM((heads // 2, 128, VN), BF16)],
        flops=400_000_000,
    )
    part, sent = call(
        project_kernel,
        "project",
        (struct((half, model), F32), struct((half, model))),
        (place, gated_wide, gated_narrow, out_wide, out_narrow),
        flops=2 * rows * model * (gated_wide.shape[1] + gated_narrow.shape[1]),
    )
    resid, normed = call(
        enter_kernel,
        "enter",
        (struct((half, model)), struct((half, model))),
        (part, crossed(sent, "core", 1), stream, gain_mix[None], gain_pre[None]),
    )
    near = jnp.stack([normed] + [crossed(normed, "hi", step) for step in range(1, line)])
    far = crossed(near, "core", 1)
    up = call(
        functools.partial(up_kernel, rest=line - 1),
        "up",
        struct((line, rows, 2 * width)),
        (place, near, far, *early_all, *ups_all),
        [pltpu.VMEM((line, line, rows, 128), BF16)],
        flops=4 * line * rows * model * width,
    )
    reach = taps_gate.shape[0] - 1
    halo = lax.ppermute(up[:, rows - reach :], "lo", [(at, (at + 1) % LO) for at in range(LO)])
    own, theirs = call(
        down_kernel,
        "down",
        (struct((line, half, model), F32), struct((line, half, model))),
        (place, up, halo, columns(taps_gate, 0), columns(taps_lin, 0), *early_all, *downs_all),
        [pltpu.VMEM((2, line * half, width), BF16)],
        flops=2 * line * rows * model * width,
    )
    theirs = crossed(theirs, "core", 1)
    sums = call(
        sum_kernel,
        "sum",
        (struct((half, model), F32),) + (struct((half, model)),) * (line - 1),
        (own, theirs),
    )
    sums = [sums[0]] + [crossed(sums[step], "hi", step) for step in range(1, line)]
    return call(
        leave_kernel,
        "leave",
        struct((half, model)),
        (resid, gain_post[None], *sums),
    )


def solution(mesh):
    count, cores = mesh.shape["sp"], mesh.shape["tp"]
    line = count // LO
    fits = cores == 2 and line * LO == count and line & (line - 1) == 0 and line == LO
    outer = ("hi", "lo") if fits else ("sp",)
    inner = "core" if fits else "tp"
    rows = P(outer, inner)
    in_specs = (
        (P((*outer, inner), None),)
        + (rows,) * 8
        + (P(None, inner, outer), P(inner), P(inner), P(inner, None), P(inner, None), P(), P(), P())
        + (rows,) * 3
        + (P(None, inner), P(None, inner))
    )
    out_specs = P((*outer, inner), None)
    if fits:
        grid = Mesh(mesh.devices.reshape(line, LO, cores), ("hi", "lo", "core"))
        return jax.shard_map(fast_body, mesh=grid, in_specs=in_specs, out_specs=out_specs, check_vma=False)
    return jax.shard_map(general_body, mesh=mesh, in_specs=in_specs, out_specs=out_specs, check_vma=False)
```
